32 devices in a mesh: grp: 2 (over y), fs: 4 (over z), tp: 4 (over x, core).
Axes of the slice: x: 2, y: 2, z: 4, core: 2. Of those that a mesh axis runs over, the one named last changes fastest.
Arguments:
- tokens: bfloat16 [6144, 2048], P(('grp', 'fs')), parts along dimension 0, may hold values from -6 to 6
- pre_gain: float32 [2048], replicated, may hold values from 0.1 to 1.9
- up_weight: bfloat16 [2048, 8192], P('fs', 'tp'), may hold values from -0.125 to 0.125
- down_weight: bfloat16 [8192, 2048], P(('tp', 'fs')), as said below
- post_gain: float32 [2048], P('tp'), may hold values from 0.1 to 1.9
Outputs:
- mixed: bfloat16 [6144, 2048], P(('grp', 'fs'), 'tp'), parts along dimension 0
The draws below stay inside these ranges and needn't reach their ends.
There are 2 independent parts, one for each index of `grp`. The reference program is written for one: setup_inputs(seed, part) draws one part's arguments, and reference() takes and returns one part's arrays. A program takes and returns all parts, laid end to end along the dimension named above; an argument that names none is the same for every part. Nothing has to cross between parts.
Inputs may be any that keep to these rules, and one draw needn't show every extreme that they name: `down_weight`: a matrix whose columns fall into 4 consecutive blocks of different magnitudes.
All inputs are finite; a program needn't handle non-finite values.
Results may differ from the reference program's by a relative error of at most 0.014.
Values may be sent and summed in bfloat16 or wider, within the bound.
A program may use at most 64 MiB of HBM per device.

```python
import jax
import jax.numpy as jnp
from jax import lax

D = 2048
FF = 8192
TOKENS = 3072
N_TP = 4


def draw_down_weight(key, part):
    first, second = jax.random.split(key, 2)
    levels = jnp.exp(jnp.linspace(jnp.log(0.3), jnp.log(3.0), N_TP)).astype(jnp.float32)
    order = jax.random.permutation(first, N_TP)
    levels = levels[order]
    column_block = jnp.arange(D) // (D // N_TP)
    column_scale = levels[column_block]
    base = jax.random.normal(second, (FF, D), jnp.float32)
    return (base * column_scale[None, :] * FF ** (-0.5)).astype(jnp.bfloat16)


def shard_levels(own_key, dims, shards, low, top_value):
    gain = 1.0
    for axis_at, parts in shards:
        steps = jax.random.uniform(jax.random.fold_in(jax.random.fold_in(own_key, 6), axis_at), (parts,), jnp.float32, low / len(shards), top_value / len(shards))
        gain = gain * jnp.repeat(jnp.exp(steps), dims[axis_at] // parts).reshape((-1,) + (1,) * (len(dims) - 1 - axis_at))
    return gain


def bell_draw(key, extent, scale, bound, shards=(), held_as=jnp.bfloat16):
    entries = jax.random.normal(key, extent, jnp.float32) * scale
    if len(shards) > 0:
        entries = shard_levels(key, extent, shards, -0.22, 0.18) * entries
    return jnp.clip(entries, min=-bound, max=bound).astype(held_as)


def setup_inputs(seed: int = 0, part: int = 0) -> dict:
    key_of = jax.random.split(jax.random.key(seed), 6)
    part_keys = jax.random.split(jax.random.fold_in(key_of[5], part), 6)
    tokens = bell_draw(part_keys[0], (TOKENS, D), 1.0, 6.0, ((0, 4),))
    pre_gain = jnp.clip(1.0 + 0.18 * jax.random.normal(key_of[1], (D,), jnp.float32), 0.1, 1.9)
    up_weight = bell_draw(key_of[2], (D, FF), D ** -0.5, 0.125, ((0, 4), (1, 4)))
    down_weight = draw_down_weight(jax.random.fold_in(key_of[5], 71), part)
    post_gain = jnp.clip(1.0 + 0.18 * jax.random.normal(key_of[4], (D,), jnp.float32), 0.1, 1.9)
    return {"tokens": tokens, "pre_gain": pre_gain, "up_weight": up_weight, "down_weight": down_weight, "post_gain": post_gain}


def reference(tokens, pre_gain, up_weight, down_weight, post_gain):
    eps = 1e-06
    values = tokens.astype(jnp.float32)
    normed = (values * lax.rsqrt(lax.optimization_barrier(jnp.mean(values * values, axis=1, keepdims=True)) + eps) * pre_gain).astype(jnp.bfloat16)
    block = FF // N_TP
    total = jnp.zeros((tokens.shape[0], D), jnp.float32)
    for index in range(N_TP):
        up = jnp.dot(normed, up_weight[:, index * block:(index + 1) * block], preferred_element_type=jnp.float32)
        hidden = jnp.square(jnp.maximum(up, 0.0)).astype(jnp.bfloat16)
        part = jnp.dot(hidden, down_weight[index * block:(index + 1) * block, :], preferred_element_type=jnp.float32).astype(jnp.bfloat16)
        part = lax.optimization_barrier(part)
        total = total + part.astype(jnp.float32)
    factor = lax.rsqrt(lax.optimization_barrier(jnp.mean(total * total, axis=1, keepdims=True)) + eps)
    return (total * factor * post_gain).astype(jnp.bfloat16)
```

```python
import functools

import jax
import jax.numpy as jnp
from jax import lax
from jax.experimental import pallas as pl
from jax.experimental.pallas import tpu as pltpu
from jax.sharding import PartitionSpec as P

MESH = pl.DeviceIdType.MESH
EPS = 1e-06
LANES = 128


def layer_kernel(sizes, tok_hbm, gain_ref, up_hbm, down_hbm, out_ref,
                 tok, normed, ubuf, dbuf, hidden, sbuf, rbuf,
                 tok_sem, lup_sem, ldn_sem, zrecv, yrecv, zsend, ysend, rsend, rrecv):
    n_grp, n_fs, n_tp, p_up, p_dn, c_up = sizes
    per_grp = n_tp // n_grp
    pieces = p_up + p_dn
    grp = lax.axis_index("grp")
    me = lax.axis_index("fs")
    tp = lax.axis_index("tp")
    rows_up = up_hbm.shape[0]
    rows_dn = down_hbm.shape[0]
    own_width = p_dn * LANES

    def block(q, g, src):
        if q < p_up:
            return ubuf.at[q, g, pl.ds(pl.multiple_of(src * rows_up, rows_up), rows_up), :]
        return dbuf.at[q - p_up, g, pl.ds(pl.multiple_of(src * rows_dn, rows_dn), rows_dn), :]

    def local_copies(q, j):
        g = lax.rem(grp + j, n_grp)
        if q < p_up:
            cols = pl.ds(pl.multiple_of((q * n_grp + g) * c_up, LANES), c_up)
            return [pltpu.make_async_copy(up_hbm.at[:, cols], block(q, g, me), lup_sem.at[q, j])]
        copies = []
        for i in range(per_grp):
            start = (g * per_grp + i) * own_width + (q - p_up) * LANES
            cols = pl.ds(pl.multiple_of(start, LANES), LANES)
            dst = dbuf.at[q - p_up, g, pl.ds(pl.multiple_of(me * rows_dn, rows_dn), rows_dn),
                          pl.ds(i * LANES, LANES)]
            copies.append(pltpu.make_async_copy(
                down_hbm.at[:, cols], dst, ldn_sem.at[q - p_up, j, i]))
        return copies

    def z_copy(q, src, side):
        to = me + 1 if side else me - 1
        return pltpu.make_async_remote_copy(
            src_ref=block(q, grp, src), dst_ref=block(q, grp, src),
            send_sem=zsend.at[q, src], recv_sem=zrecv.at[q, src],
            device_id={"fs": to}, device_id_type=MESH)

    def z_own(q, side):
        to = me + 1 if side else me - 1
        return pltpu.make_async_remote_copy(
            src_ref=block(q, grp, me), dst_ref=block(q, grp, me),
            send_sem=zsend.at[q, me] if side else zsend.at[q, n_fs], recv_sem=zrecv.at[q, me],
            device_id={"fs": to}, device_id_type=MESH)

    def y_copy(q, src, j):
        to = lax.rem(grp + j, n_grp)
        return pltpu.make_async_remote_copy(
            src_ref=block(q, grp, src), dst_ref=block(q, grp, src),
            send_sem=ysend.at[q, j, src], recv_sem=yrecv.at[q, j, src],
            device_id={"grp": to}, device_id_type=MESH)

    def y_arrival(q, src, j):
        g = lax.rem(grp + n_grp - j, n_grp)
        return pltpu.make_async_remote_copy(
            src_ref=block(q, g, src), dst_ref=block(q, g, src),
            send_sem=ysend.at[q, j, src], recv_sem=yrecv.at[q, j, src],
            device_id={"grp": g}, device_id_type=MESH)

    def part_copy(q, j):
        to = lax.rem(tp + j, n_tp)
        return pltpu.make_async_remote_copy(
            src_ref=sbuf.at[q, to], dst_ref=rbuf.at[q, j - 1],
            send_sem=rsend.at[q, j - 1], recv_sem=rrecv.at[q, j - 1],
            device_id={"tp": to}, device_id_type=MESH)

    tok_copy = pltpu.make_async_copy(tok_hbm, tok, tok_sem)
    for q in range(pieces):
        for j in range(n_grp):
            for copy in local_copies(q, j):
                copy.start()
        if q == 0:
            tok_copy.start()

    barrier = pltpu.get_barrier_semaphore()

    @pl.when(me > 0)
    def _():
        pl.semaphore_signal(barrier, inc=1, device_id={"fs": me - 1}, device_id_type=MESH)

    @pl.when(me < n_fs - 1)
    def _():
        pl.semaphore_signal(barrier, inc=1, device_id={"fs": me + 1}, device_id_type=MESH)

    for j in range(1, n_grp):
        pl.semaphore_signal(barrier, inc=1, device_id={"grp": lax.rem(grp + j, n_grp)},
                            device_id_type=MESH)
    for j in range(1, n_tp):
        pl.semaphore_signal(barrier, inc=1, device_id={"tp": lax.rem(tp + j, n_tp)},
                            device_id_type=MESH)
    ends = (me == 0).astype(jnp.int32) + (me == n_fs - 1).astype(jnp.int32)
    pl.semaphore_wait(barrier, n_grp - 1 + n_tp - 1 + 2 - ends)

    def send_own(q):
        for copy in local_copies(q, 0):
            copy.wait()

        @pl.when(me < n_fs - 1)
        def _():
            z_own(q, True).start()

        @pl.when(me > 0)
        def _():
            z_own(q, False).start()

    def relay(q, d):
        for side in (True, False):
            src = me - d if side else me + d

            @pl.when((src >= 0) & (src < n_fs))
            def _(src=src, side=side):
                z_copy(q, src, side).wait_recv()

                @pl.when(me < n_fs - 1 if side else me > 0)
                def _():
                    z_copy(q, src, side).start()

                for j in range(1, n_grp):
                    y_copy(q, src, j).start()

    def norm_tokens():
        tok_copy.wait()
        step = 64

        @pl.loop(0, tok.shape[0] // step)
        def _(r):
            at = pl.ds(pl.multiple_of(r * step, step), step)
            values = tok[at, :].astype(jnp.float32)
            scale = lax.rsqrt(jnp.mean(values * values, axis=1, keepdims=True) + EPS)
            normed[at, :] = (values * scale * gain_ref[...]).astype(jnp.bfloat16)

    def compute(q):
        for j in range(1, n_grp):
            for copy in local_copies(q, j):
                copy.wait()
            for src in range(n_fs):
                @pl.when(src != me)
                def _():
                    y_arrival(q, src, j).wait_recv()
        for g in range(n_grp):
            if q < p_up:
                up = jnp.dot(normed[...], ubuf[q, g], preferred_element_type=jnp.float32)
                at = (q * n_grp + g) * c_up
                hidden[:, at:at + c_up] = jnp.square(jnp.maximum(up, 0.0)).astype(jnp.bfloat16)
            else:
                part = jnp.dot(hidden[...], dbuf[q - p_up, g], preferred_element_type=jnp.float32)
                part = part.astype(jnp.bfloat16)
                for i in range(per_grp):
                    sbuf[q - p_up, g * per_grp + i] = part[:, i * LANES:(i + 1) * LANES]
        if q >= p_up:
            for j in range(1, n_tp):
                part_copy(q - p_up, j).start()

    def finish(q):
        total = sbuf[q, tp].astype(jnp.float32)
        for j in range(1, n_tp):
            part_copy(q, j).wait_recv()
            total = total + rbuf[q, j - 1].astype(jnp.float32)
        out_ref[:, q * LANES:(q + 1) * LANES] = total

    lag = n_fs + 1
    for k in range(pieces + lag):
        if k < pieces:
            send_own(k)
        for q in range(pieces):
            if 1 <= k - q <= n_fs - 1:
                relay(q, k - q)
        if k == 1:
            norm_tokens()
        if 0 <= k - lag < pieces:
            compute(k - lag)
        if k - lag - 1 >= p_up:
            finish(k - lag - 1 - p_up)
    finish(p_dn - 1)

    for q in range(pieces):
        @pl.when(me < n_fs - 1)
        def _():
            z_own(q, True).wait_send()

        @pl.when(me > 0)
        def _():
            z_own(q, False).wait_send()

        for d in range(1, n_fs):
            for side in (True, False):
                src = me - d if side else me + d

                @pl.when((src >= 0) & (src < n_fs))
                def _(src=src, side=side):
                    @pl.when(me < n_fs - 1 if side else me > 0)
                    def _():
                        z_copy(q, src, side).wait_send()

                    for j in range(1, n_grp):
                        y_copy(q, src, j).wait_send()
    for q in range(p_dn):
        for j in range(1, n_tp):
            part_copy(q, j).wait_send()


def shards(n_grp, n_fs, n_tp, tokens, pre_gain, up_weight, down_weight, post_gain):
    rows, width = tokens.shape
    own_width = post_gain.shape[0]
    ff = up_weight.shape[1]
    c_up = min(2 * LANES, ff // n_grp)
    p_up = ff // (n_grp * c_up)
    p_dn = own_width // LANES
    c_dn = n_tp // n_grp * LANES
    pieces = p_up + p_dn
    sizes = (n_grp, n_fs, n_tp, p_up, p_dn, c_up)
    vmem = pltpu.VMEM
    dma = pltpu.SemaphoreType.DMA
    total = pl.pallas_call(
        functools.partial(layer_kernel, sizes),
        out_shape=jax.ShapeDtypeStruct((rows, own_width), jnp.float32),
        in_specs=[
            pl.BlockSpec(memory_space=pl.ANY),
            pl.BlockSpec(memory_space=pltpu.VMEM),
            pl.BlockSpec(memory_space=pl.ANY),
            pl.BlockSpec(memory_space=pl.ANY),
        ],
        out_specs=pl.BlockSpec(memory_space=pltpu.VMEM),
        scratch_shapes=[
            vmem((rows, width), jnp.bfloat16),
            vmem((rows, width), jnp.bfloat16),
            vmem((p_up, n_grp, width, c_up), jnp.bfloat16),
            vmem((p_dn, n_grp, ff, c_dn), jnp.bfloat16),
            vmem((rows, ff), jnp.bfloat16),
            vmem((p_dn, n_tp, rows, LANES), jnp.bfloat16),
            vmem((p_dn, n_tp - 1, rows, LANES), jnp.bfloat16),
            dma,
            dma((p_up, n_grp)),
            dma((p_dn, n_grp, n_tp // n_grp)),
            dma((pieces, n_fs)),
            dma((pieces, n_grp, n_fs)),
            dma((pieces, n_fs + 1)),
            dma((pieces, n_grp, n_fs)),
            dma((p_dn, n_tp - 1)),
            dma((p_dn, n_tp - 1)),
        ],
        compiler_params=pltpu.CompilerParams(
            collective_id=0, has_side_effects=True, vmem_limit_bytes=60 * 1024 * 1024),
        cost_estimate=pl.CostEstimate(
            flops=4 * rows * width * ff, bytes_accessed=16 * rows * width, transcendentals=rows),
    )(tokens, pre_gain.reshape(1, -1), up_weight, down_weight)
    squares = lax.psum(jnp.sum(total * total, axis=1), "tp")
    factor = lax.rsqrt(squares / (n_tp * own_width) + EPS)
    return (total * factor[:, None] * post_gain).astype(jnp.bfloat16)


def solution(mesh):
    in_specs = (P(("grp", "fs"), None), P(), P("fs", "tp"), P(("tp", "fs"), None), P("tp"))
    out_specs = P(("grp", "fs"), "tp")
    body = functools.partial(shards, mesh.shape["grp"], mesh.shape["fs"], mesh.shape["tp"])
    return jax.shard_map(body, mesh=mesh, in_specs=in_specs, out_specs=out_specs, check_vma=False)
```

```python
import functools

import jax
import jax.numpy as jnp
from jax import lax
from jax.experimental import pallas as pl
from jax.experimental.pallas import tpu as pltpu
from jax.sharding import PartitionSpec as P

MESH = pl.DeviceIdType.MESH
EPS = 1e-06
LANES = 128


def layer_kernel(sizes, tok_hbm, gain_ref, up_hbm, down_hbm, post_ref, out_ref,
                 tok, normed, ubuf, dbuf, hidden, sbuf, rbuf, total_buf, square_buf, own_sq, peer_sq,
                 tok_sem, lup_sem, ldn_sem, zrecv, yrecv, zsend, ysend, rsend, rrecv,
                 sq_send, sq_recv):
    n_grp, n_fs, n_tp, p_up, p_dn, c_up, splits = sizes
    per_grp = n_tp // n_grp
    pieces = p_up + p_dn
    grp = lax.axis_index("grp")
    me = lax.axis_index("fs")
    tp = lax.axis_index("tp")
    rows_up = up_hbm.shape[0]
    rows_dn = down_hbm.shape[0]
    own_width = p_dn * LANES

    def block(q, g, src):
        if q < p_up:
            return ubuf.at[q, g, pl.ds(pl.multiple_of(src * rows_up, rows_up), rows_up), :]
        return dbuf.at[q - p_up, g, pl.ds(pl.multiple_of(src * rows_dn, rows_dn), rows_dn), :]

    def local_copies(q, j):
        g = lax.rem(grp + j, n_grp)
        if q < p_up:
            cols = pl.ds(pl.multiple_of((q * n_grp + g) * c_up, LANES), c_up)
            return [pltpu.make_async_copy(up_hbm.at[:, cols], block(q, g, me), lup_sem.at[q, j])]
        copies = []
        for i in range(per_grp):
            start = (g * per_grp + i) * own_width + (q - p_up) * LANES
            cols = pl.ds(pl.multiple_of(start, LANES), LANES)
            dst = dbuf.at[q - p_up, g, pl.ds(pl.multiple_of(me * rows_dn, rows_dn), rows_dn),
                          pl.ds(i * LANES, LANES)]
            copies.append(pltpu.make_async_copy(
                down_hbm.at[:, cols], dst, ldn_sem.at[q - p_up, j, i]))
        return copies

    def z_copy(q, src, side):
        to = me + 1 if side else me - 1
        return pltpu.make_async_remote_copy(
            src_ref=block(q, grp, src), dst_ref=block(q, grp, src),
            send_sem=zsend.at[q, src], recv_sem=zrecv.at[q, src],
            device_id={"fs": to}, device_id_type=MESH)

    def z_own(q, side):
        to = me + 1 if side else me - 1
        return pltpu.make_async_remote_copy(
            src_ref=block(q, grp, me), dst_ref=block(q, grp, me),
            send_sem=zsend.at[q, me] if side else zsend.at[q, n_fs], recv_sem=zrecv.at[q, me],
            device_id={"fs": to}, device_id_type=MESH)

    def y_copy(q, src, j):
        to = lax.rem(grp + j, n_grp)
        return pltpu.make_async_remote_copy(
            src_ref=block(q, grp, src), dst_ref=block(q, grp, src),
            send_sem=ysend.at[q, j, src], recv_sem=yrecv.at[q, j, src],
            device_id={"grp": to}, device_id_type=MESH)

    def y_arrival(q, src, j):
        g = lax.rem(grp + n_grp - j, n_grp)
        return pltpu.make_async_remote_copy(
            src_ref=block(q, g, src), dst_ref=block(q, g, src),
            send_sem=ysend.at[q, j, src], recv_sem=yrecv.at[q, j, src],
            device_id={"grp": g}, device_id_type=MESH)

    def row_blocks(q):
        count = splits if q == p_dn - 1 else 1
        height = tok.shape[0] // count
        return [(b, pl.ds(b * height, height)) for b in range(count)]

    def part_copy(q, j, b, at):
        to = lax.rem(tp + j, n_tp)
        return pltpu.make_async_remote_copy(
            src_ref=sbuf.at[q, to, at, :], dst_ref=rbuf.at[q, j - 1, at, :],
            send_sem=rsend.at[q, j - 1, b], recv_sem=rrecv.at[q, j - 1, b],
            device_id={"tp": to}, device_id_type=MESH)

    def square_copy(j):
        return pltpu.make_async_remote_copy(
            src_ref=own_sq, dst_ref=peer_sq.at[j - 1],
            send_sem=sq_send.at[j - 1], recv_sem=sq_recv.at[j - 1],
            device_id={"tp": lax.rem(tp + j, n_tp)}, device_id_type=MESH)

    tok_copy = pltpu.make_async_copy(tok_hbm, tok, tok_sem)
    for q in range(pieces):
        for j in range(n_grp):
            for copy in local_copies(q, j):
                copy.start()
        if q == 0:
            tok_copy.start()

    barrier = pltpu.get_barrier_semaphore()

    @pl.when(me > 0)
    def _():
        pl.semaphore_signal(barrier, inc=1, device_id={"fs": me - 1}, device_id_type=MESH)

    @pl.when(me < n_fs - 1)
    def _():
        pl.semaphore_signal(barrier, inc=1, device_id={"fs": me + 1}, device_id_type=MESH)

    for j in range(1, n_grp):
        pl.semaphore_signal(barrier, inc=1, device_id={"grp": lax.rem(grp + j, n_grp)},
                            device_id_type=MESH)
    for j in range(1, n_tp):
        pl.semaphore_signal(barrier, inc=1, device_id={"tp": lax.rem(tp + j, n_tp)},
                            device_id_type=MESH)
    ends = (me == 0).astype(jnp.int32) + (me == n_fs - 1).astype(jnp.int32)
    pl.semaphore_wait(barrier, n_grp - 1 + n_tp - 1 + 2 - ends)

    def send_own(q):
        for copy in local_copies(q, 0):
            copy.wait()

        @pl.when(me < n_fs - 1)
        def _():
            z_own(q, True).start()

        @pl.when(me > 0)
        def _():
            z_own(q, False).start()

    def relay(q, d):
        for side in (True, False):
            src = me - d if side else me + d

            @pl.when((src >= 0) & (src < n_fs))
            def _(src=src, side=side):
                z_copy(q, src, side).wait_recv()

                @pl.when(me < n_fs - 1 if side else me > 0)
                def _():
                    z_copy(q, src, side).start()

                for j in range(1, n_grp):
                    y_copy(q, src, j).start()

    def norm_tokens():
        tok_copy.wait()
        step = 64

        @pl.loop(0, tok.shape[0] // step)
        def _(r):
            at = pl.ds(pl.multiple_of(r * step, step), step)
            values = tok[at, :].astype(jnp.float32)
            scale = lax.rsqrt(jnp.mean(values * values, axis=1, keepdims=True) + EPS)
            normed[at, :] = (values * scale * gain_ref[...]).astype(jnp.bfloat16)

    def compute(q):
        for j in range(1, n_grp):
            for copy in local_copies(q, j):
                copy.wait()
            for src in range(n_fs):
                @pl.when(src != me)
                def _():
                    y_arrival(q, src, j).wait_recv()
        if q < p_up:
            for g in range(n_grp):
                up = jnp.dot(normed[...], ubuf[q, g], preferred_element_type=jnp.float32)
                at = (q * n_grp + g) * c_up
                hidden[:, at:at + c_up] = jnp.square(jnp.maximum(up, 0.0)).astype(jnp.bfloat16)
            return
        blocks = row_blocks(q - p_up)
        for b, at in blocks:
            for g in range(n_grp):
                part = jnp.dot(hidden[at, :], dbuf[q - p_up, g], preferred_element_type=jnp.float32)
                part = part.astype(jnp.bfloat16)
                for i in range(per_grp):
                    sbuf[q - p_up, g * per_grp + i, at, :] = part[:, i * LANES:(i + 1) * LANES]
            if b > 0:
                for j in range(1, n_tp):
                    part_copy(q - p_up, j, *blocks[b - 1]).start()
        for j in range(1, n_tp):
            part_copy(q - p_up, j, *blocks[-1]).start()

    def finish(q):
        for b, at in row_blocks(q):
            total = sbuf[q, tp, at, :].astype(jnp.float32)
            for j in range(1, n_tp):
                part_copy(q, j, b, at).wait_recv()
                total = total + rbuf[q, j - 1, at, :].astype(jnp.float32)
            total_buf[at, q * LANES:(q + 1) * LANES] = total
            square = total * total
            square_buf[at, :] = square if q == 0 else square_buf[at, :] + square

    lag = n_fs
    for k in range(pieces + lag):
        if k < pieces:
            send_own(k)
        for q in range(pieces):
            if 1 <= k - q <= n_fs - 1:
                relay(q, k - q)
        if k == 1:
            norm_tokens()
        if 0 <= k - lag < pieces:
            compute(k - lag)
        if k - lag - 1 >= p_up:
            finish(k - lag - 1 - p_up)
    finish(p_dn - 1)

    rows = tok.shape[0]
    own = jnp.sum(square_buf[...].T, axis=0, keepdims=True)
    own_sq[...] = jnp.broadcast_to(own, own_sq.shape)
    for j in range(1, n_tp):
        square_copy(j).start()
    squares = own_sq[...]
    for j in range(1, n_tp):
        square_copy(j).wait_recv()
        squares = squares + peer_sq[j - 1]
    factor = lax.rsqrt(squares / (n_tp * own_width) + EPS)
    factor = jnp.broadcast_to(factor[0:1, :], (LANES, rows)).T
    for q in range(p_dn):
        at = slice(q * LANES, (q + 1) * LANES)
        out_ref[:, at] = (total_buf[:, at] * factor * post_ref[:, at]).astype(out_ref.dtype)

    for q in range(pieces):
        @pl.when(me < n_fs - 1)
        def _():
            z_own(q, True).wait_send()

        @pl.when(me > 0)
        def _():
            z_own(q, False).wait_send()

        for d in range(1, n_fs):
            for side in (True, False):
                src = me - d if side else me + d

                @pl.when((src >= 0) & (src < n_fs))
                def _(src=src, side=side):
                    @pl.when(me < n_fs - 1 if side else me > 0)
                    def _():
                        z_copy(q, src, side).wait_send()

                    for j in range(1, n_grp):
                        y_copy(q, src, j).wait_send()
    for q in range(p_dn):
        for j in range(1, n_tp):
            for b, at in row_blocks(q):
                part_copy(q, j, b, at).wait_send()
    for j in range(1, n_tp):
        square_copy(j).wait_send()


def shards(n_grp, n_fs, n_tp, tokens, pre_gain, up_weight, down_weight, post_gain):
    rows, width = tokens.shape
    own_width = post_gain.shape[0]
    ff = up_weight.shape[1]
    c_up = min(2 * LANES, ff // n_grp)
    p_up = ff // (n_grp * c_up)
    p_dn = own_width // LANES
    c_dn = n_tp // n_grp * LANES
    pieces = p_up + p_dn
    splits = 1
    sizes = (n_grp, n_fs, n_tp, p_up, p_dn, c_up, splits)
    vmem = pltpu.VMEM
    dma = pltpu.SemaphoreType.DMA
    return pl.pallas_call(
        functools.partial(layer_kernel, sizes),
        out_shape=jax.ShapeDtypeStruct((rows, own_width), jnp.bfloat16),
        in_specs=[
            pl.BlockSpec(memory_space=pl.ANY),
            pl.BlockSpec(memory_space=pltpu.VMEM),
            pl.BlockSpec(memory_space=pl.ANY),
            pl.BlockSpec(memory_space=pl.ANY),
            pl.BlockSpec(memory_space=pltpu.VMEM),
        ],
        out_specs=pl.BlockSpec(memory_space=pltpu.VMEM),
        scratch_shapes=[
            vmem((rows, width), jnp.bfloat16),
            vmem((rows, width), jnp.bfloat16),
            vmem((p_up, n_grp, width, c_up), jnp.bfloat16),
            vmem((p_dn, n_grp, ff, c_dn), jnp.bfloat16),
            vmem((rows, ff), jnp.bfloat16),
            vmem((p_dn, n_tp, rows, LANES), jnp.bfloat16),
            vmem((p_dn, n_tp - 1, rows, LANES), jnp.bfloat16),
            vmem((rows, own_width), jnp.float32),
            vmem((rows, LANES), jnp.float32),
            vmem((8, rows), jnp.float32),
            vmem((n_tp - 1, 8, rows), jnp.float32),
            dma,
            dma((p_up, n_grp)),
            dma((p_dn, n_grp, n_tp // n_grp)),
            dma((pieces, n_fs)),
            dma((pieces, n_grp, n_fs)),
            dma((pieces, n_fs + 1)),
            dma((pieces, n_grp, n_fs)),
            dma((p_dn, n_tp - 1, splits)),
            dma((p_dn, n_tp - 1, splits)),
            dma((n_tp - 1,)),
            dma((n_tp - 1,)),
        ],
        compiler_params=pltpu.CompilerParams(
            collective_id=0, has_side_effects=True, vmem_limit_bytes=60 * 1024 * 1024),
        cost_estimate=pl.CostEstimate(
            flops=4 * rows * width * ff, bytes_accessed=16 * rows * width, transcendentals=rows),
    )(tokens, pre_gain.reshape(1, -1), up_weight, down_weight, post_gain.reshape(1, -1))


def solution(mesh):
    in_specs = (P(("grp", "fs"), None), P(), P("fs", "tp"), P(("tp", "fs"), None), P("tp"))
    out_specs = P(("grp", "fs"), "tp")
    body = functools.partial(shards, mesh.shape["grp"], mesh.shape["fs"], mesh.shape["tp"])
    return jax.shard_map(body, mesh=mesh, in_specs=in_specs, out_specs=out_specs, check_vma=False)
```
